32 devices in a mesh: grp: 2 (over y), sp: 4 (over z), tp: 4 (over x, core).
Axes of the slice: x: 2, y: 2, z: 4, core: 2. Of those that a mesh axis runs over, the one named last changes fastest.
Arguments:
- latent: bfloat16 [2048, 2048], P(('grp', 'sp', 'tp')), parts along dimension 0, may hold values from -6 to 6
- cond: bfloat16 [4096], P(('grp', 'sp')), parts along dimension 0, may hold values from -6 to 6
- context: bfloat16 [512, 2048], P(('grp', 'sp')), parts along dimension 0, may hold values from -6 to 6
- context_cond: bfloat16 [2048], P('sp'), may hold values from -6 to 6
- norm_gain: bfloat16 [2048], replicated, may hold values from 0.099609375 to 1.8984375
- mod_shift: bfloat16 [2048, 2048], P('sp', 'tp'), may hold values from -0.125 to 0.125
- mod_scale: bfloat16 [2048, 2048], P('sp', 'tp'), may hold values from -0.125 to 0.125
- mod_gate: bfloat16 [2048, 2048], P('sp', 'tp'), may hold values from -0.125 to 0.125
- w_query: bfloat16 [2048, 2048], P(None, 'tp'), may hold values from -0.125 to 0.125
- w_key: bfloat16 [2048, 2048], P(None, 'tp'), may hold values from -0.125 to 0.125
- w_value: bfloat16 [2048, 4096], P(None, 'tp'), may hold values from -0.125 to 0.125
- w_gate: bfloat16 [2048, 4096], P(None, 'tp'), may hold values from -0.125 to 0.125
- w_out: bfloat16 [4096, 2048], P('tp'), may hold values from -0.09375 to 0.09375
- decay_rate: float32 [2, 8], P(None, 'tp'), may hold values from 0.00015625 to 0.034
- context_gain: float32 [8], P('tp'), may hold values from 3 to 10
Outputs:
- mixed: bfloat16 [2048, 2048], P(('grp', 'sp', 'tp')), parts along dimension 0
The draws below stay inside these ranges and needn't reach their ends.
There are 2 independent parts, one for each index of `grp`. The reference program is written for one: setup_inputs(seed, part) draws one part's arguments, and reference() takes and returns one part's arrays. A program takes and returns all parts, laid end to end along the dimension named above; an argument that names none is the same for every part. Nothing has to cross between parts.
All inputs are finite; a program needn't handle non-finite values.
Results may differ from the reference program's by a relative error of at most 0.009.
Values may be sent and summed in bfloat16 or wider, within the bound.
No kernel may reach another device: no remote copies, remote signals or barrier semaphores. Data moves between devices by JAX's collectives and lax.ppermute only.
A program may use at most 128 MiB of HBM per device.

```python
import math
import jax
import jax.numpy as jnp
from jax import lax

D = 2048
H = 8
DK = 256
DV = 512
GRID_W = 128
BLOCK = 128
NL = 1024
CTX = 256
N_TP = 4


def draw_decay_rate(key, part):
    base = jax.random.fold_in(key, 17)
    pick_key, fast_key, slow_key = jax.random.split(base, 3)
    share = 0.5
    fast = jax.random.uniform(pick_key, (2, H), jnp.float32) < share
    fast_rate = jnp.exp(jax.random.uniform(fast_key, (2, H), jnp.float32, math.log(1.0 / 100.0), math.log(1.0 / 30.0)))
    slow_rate = jnp.exp(jax.random.uniform(slow_key, (2, H), jnp.float32, math.log(0.2), math.log(2.0))) / (NL + CTX)
    return jnp.where(fast, fast_rate, slow_rate).astype(jnp.float32)


def level_of(rng, extent, cuts, low, high):
    factor_of = 1.0
    for position, shards_of in cuts:
        heights = jax.random.uniform(jax.random.fold_in(jax.random.fold_in(rng, 6), position), (shards_of,), jnp.float32, low / len(cuts), high / len(cuts))
        factor_of = factor_of * jnp.repeat(jnp.exp(heights), extent[position] // shards_of).reshape((-1,) + (1,) * (len(extent) - 1 - position))
    return factor_of


def gaussian(key, shape, scale, reach, cuts=(), kind=jnp.bfloat16):
    entries = scale * jax.random.normal(key, shape, jnp.float32)
    if cuts:
        entries = entries * level_of(key, shape, cuts, -0.22, 0.18)
    return jnp.clip(entries, -reach, reach).astype(kind)


def setup_inputs(seed: int = 0, part: int = 0) -> dict:
    arg_keys = jax.random.split(jax.random.key(seed), 16)
    own_keys = jax.random.split(jax.random.fold_in(arg_keys[15], part), 16)
    latent = gaussian(own_keys[0], (NL, D), 1.0, 6.0, ((0, 16),))
    cond = gaussian(own_keys[1], (D,), 1.0, 6.0, ((0, 4),))
    context = gaussian(own_keys[2], (CTX, D), 1.0, 6.0, ((0, 4),))
    context_cond = gaussian(arg_keys[3], (D,), 1.0, 6.0, ((0, 4),))
    norm_gain = jnp.clip(1.0 + 0.18 * jax.random.normal(arg_keys[4], (D,), jnp.float32), 0.099609375, 1.8984375).astype(jnp.bfloat16)
    mod_shift = gaussian(arg_keys[5], (D, D), D ** -0.5, 0.125, ((0, 4), (1, 4)))
    mod_scale = gaussian(arg_keys[6], (D, D), D ** -0.5, 0.125, ((0, 4), (1, 4)))
    mod_gate = gaussian(arg_keys[7], (D, D), D ** -0.5, 0.125, ((0, 4), (1, 4)))
    w_query = gaussian(arg_keys[8], (D, H * DK), D ** -0.5, 0.125, ((1, 4),))
    w_key = gaussian(arg_keys[9], (D, H * DK), D ** -0.5, 0.125, ((1, 4),))
    w_value = gaussian(arg_keys[10], (D, H * DV), D ** -0.5, 0.125, ((1, 4),))
    w_gate = gaussian(arg_keys[11], (D, H * DV), D ** -0.5, 0.125, ((1, 4),))
    w_out = gaussian(arg_keys[12], (H * DV, D), (H * DV) ** -0.5, 0.09375, ((0, 4),))
    decay_rate = draw_decay_rate(jax.random.fold_in(arg_keys[15], 71), part)
    context_gain = jnp.clip(jnp.exp(math.log(10.0) - 1.2039728 * jax.random.uniform(arg_keys[14], (H,), jnp.float32) ** level_of(arg_keys[14], (H,), ((0, 4),), -0.2, 0.2)), 3.0, 10.0)
    return {"latent": latent, "cond": cond, "context": context, "context_cond": context_cond, "norm_gain": norm_gain, "mod_shift": mod_shift, "mod_scale": mod_scale, "mod_gate": mod_gate, "w_query": w_query, "w_key": w_key, "w_value": w_value, "w_gate": w_gate, "w_out": w_out, "decay_rate": decay_rate, "context_gain": context_gain}


norm_eps = 1e-06
rope_base = 10000.0
highest = lax.Precision.HIGHEST

def modulated(rows, norm_gain, shift, scale):
    values = rows.astype(jnp.float32)
    normed = values * lax.rsqrt(lax.optimization_barrier(jnp.mean(values * values, axis=-1, keepdims=True)) + norm_eps)
    return (normed * norm_gain.astype(jnp.float32) * (1.0 + scale) + shift).astype(jnp.bfloat16)

def rotate(vectors, positions):
    depth = vectors.shape[-1]
    freqs = depth // 4
    inv_freq = rope_base ** (-jnp.arange(freqs, dtype=jnp.float32) / freqs)
    grid_row = (positions // GRID_W).astype(jnp.float32)
    grid_col = (positions % GRID_W).astype(jnp.float32)
    angles = jnp.concatenate([grid_row[:, None] * inv_freq, grid_col[:, None] * inv_freq], axis=-1)[:, None, :]
    cos_table = jnp.cos(angles)
    sin_table = jnp.sin(angles)
    first_half, second_half = jnp.split(vectors, 2, axis=-1)
    return jnp.concatenate([first_half * cos_table - second_half * sin_table, second_half * cos_table + first_half * sin_table], axis=-1)

def rounded(values):
    return lax.optimization_barrier(values.astype(jnp.bfloat16)).astype(jnp.float32)

def context_states(ctx_key, ctx_value, fwd_rate, bwd_rate, context_gain):
    total = ctx_key.shape[0]
    place = jnp.arange(total, dtype=jnp.float32)[:, None]
    fwd_weight = jnp.exp(-fwd_rate[None, :] * (total - 1.0 - place))
    bwd_weight = jnp.exp(-bwd_rate[None, :] * place)
    keys_f = lax.optimization_barrier(ctx_key).astype(jnp.float32)
    values_f = lax.optimization_barrier(ctx_value).astype(jnp.float32)
    fwd_keys = rounded(keys_f * fwd_weight[:, :, None])
    bwd_keys = rounded(keys_f * bwd_weight[:, :, None])
    fwd_state = jnp.einsum('jhd,jhe->hde', fwd_keys, values_f, precision=highest)
    bwd_state = jnp.einsum('jhd,jhe->hde', bwd_keys, values_f, precision=highest)
    return (fwd_state * context_gain[:, None, None], bwd_state * context_gain[:, None, None])

def reference(latent, cond, context, context_cond, norm_gain, mod_shift, mod_scale, mod_gate, w_query, w_key, w_value, w_gate, w_out, decay_rate, context_gain):
    cond_rows = jax.nn.silu(jnp.stack([cond, context_cond]).astype(jnp.float32)).astype(jnp.bfloat16)
    shift = jnp.dot(cond_rows, mod_shift, preferred_element_type=jnp.float32)
    scale = jnp.dot(cond_rows, mod_scale, preferred_element_type=jnp.float32)
    gate = jnp.dot(cond_rows[0:1], mod_gate, preferred_element_type=jnp.float32)
    h_latent = modulated(latent, norm_gain, shift[0], scale[0])
    h_context = modulated(context, norm_gain, shift[1], scale[1])
    positions = jnp.arange(NL, dtype=jnp.int32)
    query = rotate(jnp.dot(h_latent, w_query, preferred_element_type=jnp.float32).reshape(NL, H, DK), positions).astype(jnp.bfloat16)
    keys = rotate(jnp.dot(h_latent, w_key, preferred_element_type=jnp.float32).reshape(NL, H, DK) * DK ** (-0.5), positions).astype(jnp.bfloat16)
    values = jnp.dot(h_latent, w_value, preferred_element_type=jnp.float32).astype(jnp.bfloat16).reshape(NL, H, DV)
    gate_pre = jnp.dot(h_latent, w_gate, preferred_element_type=jnp.float32).reshape(NL, H, DV)
    ctx_key = (jnp.dot(h_context, w_key, preferred_element_type=jnp.float32) * DK ** (-0.5)).astype(jnp.bfloat16)
    ctx_value = jnp.dot(h_context, w_value, preferred_element_type=jnp.float32).astype(jnp.bfloat16)
    fwd_rate = decay_rate[0]
    bwd_rate = decay_rate[1]
    ctx_fwd, ctx_bwd = context_states(ctx_key.reshape(CTX, H, DK), ctx_value.reshape(CTX, H, DV), fwd_rate, bwd_rate, context_gain)
    blocks = NL // BLOCK
    query_f = lax.optimization_barrier(query).astype(jnp.float32).reshape(blocks, BLOCK, H, DK)
    keys_f = lax.optimization_barrier(keys).astype(jnp.float32).reshape(blocks, BLOCK, H, DK)
    values_f = lax.optimization_barrier(values).astype(jnp.float32).reshape(blocks, BLOCK, H, DV)
    place = jnp.arange(BLOCK, dtype=jnp.float32)
    gap = place[:, None] - place[None, :]
    mask = jnp.where(gap >= 0, jnp.exp(-fwd_rate[:, None, None] * jnp.maximum(gap, 0.0)), 0.0) + jnp.where(gap <= 0, jnp.exp(-bwd_rate[:, None, None] * jnp.maximum(-gap, 0.0)), 0.0)
    scores = jnp.einsum('bihd,bjhd->bhij', query_f, keys_f, precision=highest)
    weights = lax.optimization_barrier((scores * mask[None]).astype(jnp.bfloat16)).astype(jnp.float32)
    retained = jnp.einsum('bhij,bjhe->bihe', weights, values_f, precision=highest)
    fwd_qw = jnp.exp(-fwd_rate[None, :] * (place[:, None] + 1.0))
    bwd_qw = jnp.exp(-bwd_rate[None, :] * (BLOCK - place[:, None]))
    fwd_kw = jnp.exp(-fwd_rate[None, :] * (BLOCK - 1.0 - place[:, None]))
    bwd_kw = jnp.exp(-bwd_rate[None, :] * place[:, None])
    fwd_keys = rounded(keys_f * fwd_kw[None, :, :, None])
    bwd_keys = rounded(keys_f * bwd_kw[None, :, :, None])
    fwd_step_decay = jnp.exp(-fwd_rate * BLOCK)[:, None, None]
    bwd_step_decay = jnp.exp(-bwd_rate * BLOCK)[:, None, None]

    def fwd_step(state, block):
        block_query, block_keys, block_values = block
        cross = jnp.einsum('ihd,hde->ihe', block_query, rounded(state), precision=highest) * fwd_qw[:, :, None]
        added = jnp.einsum('jhd,jhe->hde', block_keys, block_values, precision=highest)
        return (fwd_step_decay * state + added, cross)

    def bwd_step(state, block):
        block_query, block_keys, block_values = block
        cross = jnp.einsum('ihd,hde->ihe', block_query, rounded(state), precision=highest) * bwd_qw[:, :, None]
        added = jnp.einsum('jhd,jhe->hde', block_keys, block_values, precision=highest)
        return (bwd_step_decay * state + added, cross)
    fwd_final, fwd_cross = lax.scan(fwd_step, ctx_fwd, (query_f, fwd_keys, values_f))
    bwd_final, bwd_cross = lax.scan(bwd_step, ctx_bwd, (query_f, bwd_keys, values_f), reverse=True)
    retained = (retained + fwd_cross + bwd_cross).reshape(NL, H, DV)
    centre = lax.optimization_barrier(jnp.mean(retained, axis=-1, keepdims=True))
    variance = lax.optimization_barrier(jnp.mean(jnp.square(retained - centre), axis=-1, keepdims=True))
    normed = (retained - centre) * lax.rsqrt(variance + norm_eps)
    gated = (jax.nn.silu(gate_pre) * normed).astype(jnp.bfloat16).reshape(NL, H * DV)
    group_cols = H // N_TP * DV
    total = jnp.zeros((NL, D), jnp.float32)
    for group in range(N_TP):
        lower = group * group_cols
        partial_sum = jnp.dot(gated[:, lower:lower + group_cols], w_out[lower:lower + group_cols], preferred_element_type=jnp.float32).astype(jnp.bfloat16)
        total = total + lax.optimization_barrier(partial_sum).astype(jnp.float32)
    return (latent.astype(jnp.float32) + gate[0] * total).astype(jnp.bfloat16)
```

```python
import jax
import jax.numpy as jnp
from jax import lax
from jax.sharding import PartitionSpec as P

DK = 256
GRID_W = 128


norm_eps = 1e-06
rope_base = 10000.0


def swap(x, axis, d):
    if d == 0:
        return x
    return lax.ppermute(x, axis, [(i, i ^ d) for i in range(lax.axis_size(axis))])


def dot(a, b):
    return jnp.dot(a, b, preferred_element_type=jnp.float32)


def normed(rows):
    values = rows.astype(jnp.float32)
    return values * lax.rsqrt(jnp.mean(values * values, axis=-1, keepdims=True) + norm_eps)


def angles_of(positions):
    freqs = DK // 4
    inv_freq = rope_base ** (-jnp.arange(freqs, dtype=jnp.float32) / freqs)
    grid_row = (positions // GRID_W).astype(jnp.float32)
    grid_col = (positions % GRID_W).astype(jnp.float32)
    return jnp.concatenate([grid_row[:, None] * inv_freq, grid_col[:, None] * inv_freq], axis=-1)


def rotate(vectors, cos_table, sin_table):
    u, w = vectors[:, : DK // 2], vectors[:, DK // 2 :]
    return jnp.concatenate(
        [u * cos_table - w * sin_table, w * cos_table + u * sin_table], axis=-1
    ).astype(jnp.bfloat16)


def body(
    latent,
    cond,
    context,
    context_cond,
    norm_gain,
    mod_shift,
    mod_scale,
    mod_gate,
    w_query,
    w_key,
    w_value,
    w_gate,
    w_out,
    decay_rate,
    context_gain,
):
    heads = w_query.shape[1] // DK
    width = w_value.shape[1] // heads
    n_sp, n_tp = lax.axis_size("sp"), lax.axis_size("tp")
    sp, tp = lax.axis_index("sp"), lax.axis_index("tp")
    rows = latent.shape[0]
    span = rows * n_tp
    total = span * n_sp
    ctx_rows = context.shape[0] // n_tp
    ctx_span = context.shape[0]
    ctx_total = ctx_span * n_sp

    cond_rows = jax.nn.silu(jnp.stack([cond, context_cond]).astype(jnp.float32)).astype(
        jnp.bfloat16
    )
    part = jnp.concatenate(
        [dot(cond_rows, mod_shift), dot(cond_rows, mod_scale), dot(cond_rows[0:1], mod_gate)]
    )
    mod = part
    for d in range(1, n_sp):
        mod = mod + swap(part, "sp", d)

    mine = jnp.concatenate([latent, lax.dynamic_slice_in_dim(context, tp * ctx_rows, ctx_rows)])
    evens = list(range(0, n_tp, 2))
    odds = [e + 1 for e in evens]
    order = odds + evens

    def over_tp(slab):
        got = {}
        for e in evens[1:] + [0]:
            got[e] = swap(slab, "tp", e)
            got[e + 1] = swap(got[e], "tp", 1)
        pieces = [got[e] for e in order]
        return jnp.concatenate([p[:rows] for p in pieces] + [p[rows:] for p in pieces])

    own = over_tp(mine)
    mine, mod = lax.optimization_barrier((mine, mod))
    chunks = [own] + [over_tp(swap(mine, "sp", d)) for d in range(1, n_sp)]

    cols = mod.shape[1]
    full = jnp.zeros((mod.shape[0], cols * n_tp), jnp.float32)
    for e in range(n_tp):
        full = lax.dynamic_update_slice(full, swap(mod, "tp", e), (0, (tp ^ e) * cols))
    gain = norm_gain.astype(jnp.float32)
    shift, scale, gate = full[0:2], gain * (1.0 + full[2:4]), full[4:5]

    fwd_rate, bwd_rate = decay_rate[0], decay_rate[1]

    def places(d):
        far = sp ^ d
        lat = jnp.concatenate(
            [far * span + (tp ^ e) * rows + jnp.arange(rows, dtype=jnp.int32) for e in order]
        )
        ctx = jnp.concatenate(
            [
                far * ctx_span + (tp ^ e) * ctx_rows + jnp.arange(ctx_rows, dtype=jnp.int32)
                for e in order
            ]
        )
        return lat, ctx

    t = places(0)[0].astype(jnp.float32)[:, None]
    retained = [jnp.zeros((span, width), jnp.float32) for _ in range(heads)]
    query = gate_pre = None
    for d, chunk in enumerate(chunks):
        lat, ctx = places(d)
        is_ctx = (jnp.arange(chunk.shape[0]) >= span)[:, None]
        h = (
            normed(chunk) * jnp.where(is_ctx, scale[1:2], scale[0:1])
            + jnp.where(is_ctx, shift[1:2], shift[0:1])
        ).astype(jnp.bfloat16)
        angles = jnp.concatenate(
            [angles_of(lat), jnp.zeros((ctx.shape[0], DK // 2), jnp.float32)]
        )
        cos_table, sin_table = jnp.cos(angles), jnp.sin(angles)
        if d == 0:
            q = dot(h[:span], w_query)
            query = [
                rotate(q[:, i * DK : (i + 1) * DK], cos_table[:span], sin_table[:span])
                for i in range(heads)
            ]
            gate_pre = dot(h[:span], w_gate)
        k = dot(h, w_key) * DK ** (-0.5)
        v = dot(h, w_value).astype(jnp.bfloat16)
        gap = t - lat.astype(jnp.float32)[None, :]
        j = ctx.astype(jnp.float32)[None, :]
        for i in range(heads):
            a, b = fwd_rate[i], bwd_rate[i]
            mask = jnp.concatenate(
                [
                    jnp.where(gap >= 0, jnp.exp(-a * jnp.maximum(gap, 0.0)), 0.0)
                    + jnp.where(gap <= 0, jnp.exp(-b * jnp.maximum(-gap, 0.0)), 0.0),
                    context_gain[i]
                    * (jnp.exp(-a * (t + (ctx_total - j))) + jnp.exp(-b * ((total - t) + j))),
                ],
                axis=1,
            )
            key = rotate(k[:, i * DK : (i + 1) * DK], cos_table, sin_table)
            scores = lax.dot_general(
                query[i], key, (((1,), (1,)), ((), ())), preferred_element_type=jnp.float32
            )
            weights = (scores * mask).astype(jnp.bfloat16)
            retained[i] = retained[i] + dot(weights, v[:, i * width : (i + 1) * width])

    gated = []
    for i in range(heads):
        centre = jnp.mean(retained[i], axis=-1, keepdims=True)
        off = retained[i] - centre
        variance = jnp.mean(jnp.square(off), axis=-1, keepdims=True)
        gated.append(
            (jax.nn.silu(gate_pre[:, i * width : (i + 1) * width]) * off
             * lax.rsqrt(variance + norm_eps)).astype(jnp.bfloat16)
        )
    gated = jnp.concatenate(gated, axis=1)

    half = len(odds) * rows
    theirs = swap(dot(gated[:half], w_out).astype(jnp.bfloat16), "tp", 1).astype(jnp.float32)
    pair = dot(gated[half:], w_out) + theirs
    output_sum = pair[:rows]
    for n, e in enumerate(evens[1:], 1):
        output_sum = output_sum + swap(
            pair[n * rows : (n + 1) * rows].astype(jnp.bfloat16), "tp", e
        ).astype(jnp.float32)
    return (latent.astype(jnp.float32) + gate * output_sum).astype(jnp.bfloat16)


def solution(mesh):
    return jax.shard_map(
        body,
        mesh=mesh,
        in_specs=(
            P(("grp", "sp", "tp"), None),
            P(("grp", "sp")),
            P(("grp", "sp"), None),
            P("sp"),
            P(),
            P("sp", "tp"),
            P("sp", "tp"),
            P("sp", "tp"),
            P(None, "tp"),
            P(None, "tp"),
            P(None, "tp"),
            P(None, "tp"),
            P("tp", None),
            P(None, "tp"),
            P("tp"),
        ),
        out_specs=P(("grp", "sp", "tp"), None),
        check_vma=False,
    )
```

```python
import jax
import jax.numpy as jnp
from jax import lax
from jax.experimental import pallas as pl
from jax.experimental.pallas import tpu as pltpu
from jax.sharding import PartitionSpec as P

DK = 256
GRID_W = 128


norm_eps = 1e-06
rope_base = 10000.0


def swap(x, axis, d):
    if d == 0:
        return x
    return lax.ppermute(x, axis, [(i, i ^ d) for i in range(lax.axis_size(axis))])


def dot(a, b):
    return jnp.dot(a, b, preferred_element_type=jnp.float32)


def modulate(pieces, scale, shift, rows):
    extra = pieces[0].shape[0] - rows
    count = len(pieces)

    def kernel(scale_ref, shift_ref, *refs):
        out = refs[-1]
        for n in range(count):
            values = refs[n][...].astype(jnp.float32)
            mean = jnp.mean(values * values, axis=-1, keepdims=True)
            values = values * lax.rsqrt(mean + norm_eps)
            out[n * rows : (n + 1) * rows, :] = (
                values[:rows] * scale_ref[0:1, :] + shift_ref[0:1, :]
            ).astype(jnp.bfloat16)
            at = count * rows + n * extra
            out[at : at + extra, :] = (
                values[rows:] * scale_ref[1:2, :] + shift_ref[1:2, :]
            ).astype(jnp.bfloat16)

    return pl.pallas_call(
        kernel,
        out_shape=jax.ShapeDtypeStruct((count * (rows + extra), scale.shape[1]), jnp.bfloat16),
        name="modulate",
    )(scale, shift, *pieces)


def retain(rates, t, places, tables, q, gate_pre, keys, values, span, width, total, ctx_total):
    heads = rates.shape[1]
    count = len(keys)
    length = keys[0].shape[0]

    def turn(x, cos_table, sin_table):
        u, w = x[:, : DK // 2], x[:, DK // 2 :]
        return jnp.concatenate(
            [u * cos_table - w * sin_table, w * cos_table + u * sin_table], axis=-1
        ).astype(jnp.bfloat16)

    def kernel(rates_ref, t_ref, place_ref, cos_ref, sin_ref, q_ref, gate_ref, *refs):
        out = refs[-1]
        i = pl.program_id(0)
        a, b, gain = rates_ref[0, i], rates_ref[1, i], rates_ref[2, i]
        t = t_ref[...]
        query = turn(q_ref[...], cos_ref[0, :span], sin_ref[0, :span])
        kept = jnp.zeros((span, width), jnp.float32)
        for n in range(count):
            key = turn(refs[n][...], cos_ref[n], sin_ref[n])
            scores = lax.dot_general(
                query, key, (((1,), (1,)), ((), ())), preferred_element_type=jnp.float32
            )
            place = place_ref[n : n + 1, :]
            gap = t - place[:, :span]
            fall = jnp.exp(jnp.where(gap >= 0, -a, b) * gap)
            mask = jnp.where(gap == 0, 2.0, fall)
            j = place[:, span:]
            ctx_mask = gain * (jnp.exp(-a * (t + (ctx_total - j))) + jnp.exp(-b * ((total - t) + j)))
            weights = jnp.concatenate(
                [scores[:, :span] * mask, scores[:, span:] * ctx_mask], axis=1
            ).astype(jnp.bfloat16)
            kept = kept + dot(weights, refs[count + n][...])
        off = kept - jnp.mean(kept, axis=-1, keepdims=True)
        variance = jnp.mean(off * off, axis=-1, keepdims=True)
        pre = gate_ref[...]
        out[...] = (pre * (1.0 / (1.0 + jnp.exp(-pre))) * off * lax.rsqrt(variance + norm_eps)).astype(
            jnp.bfloat16
        )

    def whole(x):
        return pl.BlockSpec(x.shape, lambda i: (0,) * x.ndim)

    return pl.pallas_call(
        kernel,
        grid=(heads,),
        in_specs=[pl.BlockSpec(memory_space=pltpu.SMEM)]
        + [whole(x) for x in (t, places, *tables)]
        + [
            pl.BlockSpec((span, DK), lambda i: (0, i)),
            pl.BlockSpec((span, width), lambda i: (0, i)),
        ]
        + [pl.BlockSpec((length, DK), lambda i: (0, i))] * count
        + [pl.BlockSpec((length, width), lambda i: (0, i))] * count,
        out_specs=pl.BlockSpec((span, width), lambda i: (0, i)),
        out_shape=jax.ShapeDtypeStruct((span, heads * width), jnp.bfloat16),
        name="retain",
    )(rates, t, places, *tables, q, gate_pre, *keys, *values)


def angles_of(positions):
    freqs = DK // 4
    inv_freq = rope_base ** (-jnp.arange(freqs, dtype=jnp.float32) / freqs)
    grid_row = (positions // GRID_W).astype(jnp.float32)
    grid_col = (positions % GRID_W).astype(jnp.float32)
    return jnp.concatenate([grid_row[:, None] * inv_freq, grid_col[:, None] * inv_freq], axis=-1)


def body(
    latent,
    cond,
    context,
    context_cond,
    norm_gain,
    mod_shift,
    mod_scale,
    mod_gate,
    w_query,
    w_key,
    w_value,
    w_gate,
    w_out,
    decay_rate,
    context_gain,
):
    heads = w_query.shape[1] // DK
    width = w_value.shape[1] // heads
    n_sp, n_tp = lax.axis_size("sp"), lax.axis_size("tp")
    sp, tp = lax.axis_index("sp"), lax.axis_index("tp")
    rows = latent.shape[0]
    span = rows * n_tp
    total = span * n_sp
    ctx_rows = context.shape[0] // n_tp
    ctx_span = context.shape[0]
    ctx_total = ctx_span * n_sp

    cond_rows = jax.nn.silu(jnp.stack([cond, context_cond]).astype(jnp.float32)).astype(
        jnp.bfloat16
    )
    part = jnp.concatenate(
        [dot(cond_rows, mod_shift), dot(cond_rows, mod_scale), dot(cond_rows[0:1], mod_gate)]
    )
    mod = part
    for d in range(1, n_sp):
        mod = mod + swap(part, "sp", d)

    mine = jnp.concatenate([latent, lax.dynamic_slice_in_dim(context, tp * ctx_rows, ctx_rows)])
    evens = list(range(0, n_tp, 2))
    odds = [e + 1 for e in evens]
    order = odds + evens

    def over_tp(slab):
        got = {}
        for e in evens[1:] + [0]:
            got[e] = swap(slab, "tp", e)
            got[e + 1] = swap(got[e], "tp", 1)
        return [got[e] for e in order]

    own = over_tp(mine)
    mine, mod = lax.optimization_barrier((mine, mod))
    chunks = [own] + [over_tp(swap(mine, "sp", d)) for d in range(1, n_sp)]

    cols = mod.shape[1]
    full = jnp.zeros((mod.shape[0], cols * n_tp), jnp.float32)
    for e in range(n_tp):
        full = lax.dynamic_update_slice(full, swap(mod, "tp", e), (0, (tp ^ e) * cols))
    gain = norm_gain.astype(jnp.float32)
    shift, scale, gate = full[0:2], gain * (1.0 + full[2:4]), full[4:5]

    rates = jnp.concatenate([decay_rate, context_gain[None, :]])

    def places(d):
        far = sp ^ d
        lat = jnp.concatenate(
            [far * span + (tp ^ e) * rows + jnp.arange(rows, dtype=jnp.int32) for e in order]
        )
        ctx = jnp.concatenate(
            [
                far * ctx_span + (tp ^ e) * ctx_rows + jnp.arange(ctx_rows, dtype=jnp.int32)
                for e in order
            ]
        )
        return lat, ctx

    t = places(0)[0].astype(jnp.float32)[:, None]
    spots, angles, keys, values = [], [], [], []
    for d in range(n_sp):
        lat, ctx = places(d)
        spots.append(jnp.concatenate([lat, ctx]).astype(jnp.float32))
        angles.append(
            jnp.concatenate([angles_of(lat), jnp.zeros((ctx.shape[0], DK // 2), jnp.float32)])
        )
    angles = jnp.stack(angles)
    tables = (jnp.cos(angles), jnp.sin(angles))
    q = gate_pre = None
    for d, chunk in enumerate(chunks):
        h = modulate(chunk, scale, shift, rows)
        if d == 0:
            q = dot(h[:span], w_query)
            gate_pre = dot(h[:span], w_gate)
        keys.append(dot(h, w_key) * DK ** (-0.5))
        values.append(dot(h, w_value).astype(jnp.bfloat16))
    gated = retain(
        rates, t, jnp.stack(spots), tables, q, gate_pre, keys, values, span, width, total, ctx_total
    )

    half = len(odds) * rows
    theirs = swap(dot(gated[:half], w_out).astype(jnp.bfloat16), "tp", 1).astype(jnp.float32)
    pair = dot(gated[half:], w_out) + theirs
    output_sum = pair[:rows]
    for n, e in enumerate(evens[1:], 1):
        output_sum = output_sum + swap(
            pair[n * rows : (n + 1) * rows].astype(jnp.bfloat16), "tp", e
        ).astype(jnp.float32)
    return (latent.astype(jnp.float32) + gate * output_sum).astype(jnp.bfloat16)


def solution(mesh):
    return jax.shard_map(
        body,
        mesh=mesh,
        in_specs=(
            P(("grp", "sp", "tp"), None),
            P(("grp", "sp")),
            P(("grp", "sp"), None),
            P("sp"),
            P(),
            P("sp", "tp"),
            P("sp", "tp"),
            P("sp", "tp"),
            P(None, "tp"),
            P(None, "tp"),
            P(None, "tp"),
            P(None, "tp"),
            P("tp", None),
            P(None, "tp"),
            P("tp"),
        ),
        out_specs=P(("grp", "sp", "tp"), None),
        check_vma=False,
    )
```
